256 devices in a mesh: sp: 64 (over z, x, core), tp: 4 (over y).
Axes of the slice: x: 4, y: 4, z: 8, core: 2. Of those that a mesh axis runs over, the one named last changes fastest.
Arguments:
- queries: bfloat16 [65536, 2048], P('sp', 'tp'), may hold values from -16 to 16
- key_rows: bfloat16 [65536, 512], P('sp', 'tp'), may hold values from -16 to 16
- value_rows: bfloat16 [65536, 512], P('sp', 'tp'), may hold values from -6 to 6
- doc_ids: int32 [65536], P('sp'), may hold values from 0 to 31, never falling along the last dimension, each value on 1 to 4096 neighbouring positions
- sink_logit: float32 [32], P('tp'), may hold values from 3 to 7
- residual: bfloat16 [65536, 2048], P(('sp', 'tp')), may hold values from -6 to 6
- out_weight: bfloat16 [2048, 2048], P('tp'), may hold values from -3.5 to 3.5
- norm_gain: float32 [2048], replicated, may hold values from 0.1 to 1.9
- gate_weight: bfloat16 [64, 2048, 512], P('sp'), may hold values from -0.125 to 0.125
- up_weight: bfloat16 [64, 2048, 512], P('sp'), may hold values from -0.125 to 0.125
- down_weight: bfloat16 [64, 512, 2048], P('sp'), may hold values from -0.25 to 0.25
- routes: int32 [65536, 2], P(('sp', 'tp')), may hold values from 0 to 63, as said below
- route_weights: float32 [65536, 2], P(('sp', 'tp')), may hold values from 0.2 to 0.8
Outputs:
- mixed: bfloat16 [65536, 2048], P(('sp', 'tp'))
The draws below stay inside these ranges and needn't reach their ends.
Inputs may be any that keep to these rules, and one draw needn't show every extreme that they name: `doc_ids`: never falls along the positions. `routes`: each aligned block of 256 rows names every expert exactly 8 times; the experts of one row differ and lie in one group of 16 consecutive numbers.
All inputs are finite; a program needn't handle non-finite values.
Results may differ from the reference program's by a relative error of at most 0.012.
Values may be sent and summed in bfloat16 or wider, within the bound.
No kernel may reach another device: no remote copies, remote signals or barrier semaphores. Data moves between devices by JAX's collectives and lax.ppermute only.
A program may use at most 128 MiB of HBM per device.

```python
import math
import jax
import jax.numpy as jnp
import numpy as np
from jax import lax

D = 2048
HEADS = 32
KV_HEADS = 8
HD = 64
FF = 512
WINDOW = 128
GROUPS = 4
TOPK = 2
TOKENS = 65536
EXPERTS = 64
GROUP_SIZE = 16
ROWS_HOME = 256
CAP = 8
DOCS = 32
DOC_MOST = 4096
N_TP = 4


def draw_queries(key, part):
    noise = jax.random.truncated_normal(jax.random.fold_in(key, 11), -4.0, 4.0, (TOKENS, HEADS * HD), jnp.float32)
    return noise.astype(jnp.bfloat16)


def draw_key_rows(key, part):
    noise = jax.random.truncated_normal(jax.random.fold_in(key, 12), -4.0, 4.0, (TOKENS, KV_HEADS * HD), jnp.float32)
    return noise.astype(jnp.bfloat16)


def draw_routes(key, part):
    block_total = TOKENS // ROWS_HOME
    half_slots = GROUP_SIZE * CAP // 2

    def one_block(block_key):
        order_key, shuffle_key = jax.random.split(block_key)
        group_keys = jax.random.split(order_key, GROUPS)
        ordering = jax.vmap(lambda group_key: jax.random.permutation(group_key, GROUP_SIZE))(group_keys)
        ordering = ordering.astype(jnp.int32) + (jnp.arange(GROUPS, dtype=jnp.int32) * GROUP_SIZE)[:, None]
        slot_ids = jnp.arange(half_slots, dtype=jnp.int32)
        leading = ordering[:, slot_ids // CAP]
        trailing = ordering[:, (slot_ids + half_slots) // CAP]
        paired = jnp.stack([leading.reshape(-1), trailing.reshape(-1)], axis=1)
        shuffle = jax.random.permutation(shuffle_key, ROWS_HOME)
        return paired[shuffle].astype(jnp.int32)
    blocks = jax.vmap(one_block)(jax.random.split(jax.random.fold_in(key, 77), block_total))
    return blocks.reshape(TOKENS, TOPK)


def levels(key, shape, cuts, low, high):
    gain, own = 1.0, jax.random.fold_in(key, 6)
    for dim, blocks in cuts:
        draws = jnp.exp(jax.random.uniform(jax.random.fold_in(own, dim), (blocks,), jnp.float32, low / len(cuts), high / len(cuts)))
        gain = gain * jnp.repeat(draws, shape[dim] // blocks).reshape([-1 if axis == dim else 1 for axis in range(len(shape))])
    return gain


def split_up(number_of, total, limit, lean):
    portions = [(1 << 20) // math.isqrt(standing ** lean) + 1 for standing in range(2, number_of + 1)]
    rest, counts = total - limit - (number_of - 1), [1] * (number_of - 1)
    while rest > 0:
        candidates = [i for i in range(number_of - 1) if counts[i] < limit]
        whole, remaining = sum([portions[i] for i in candidates]), rest
        for i in candidates:
            extra = min(limit - counts[i], max(1, remaining * portions[i] // whole), rest)
            counts[i] = counts[i] + extra
            rest = rest - extra
    return np.array([limit] + counts)


def uneven(own_key, number_of, total, bound, skew):
    if number_of == 2:
        one = jax.random.randint(own_key, (), max(1, total - bound), min(bound, total - 1) + 1)
        return jnp.stack([one, total - one])
    lengths = jnp.asarray(split_up(number_of, total, bound, skew), jnp.int32)
    pairs = (number_of - 1) // 2
    giver, taker = lengths[1:1 + 2 * pairs:2], lengths[2:2 + 2 * pairs:2]
    margin = jnp.minimum(giver - 1, bound - taker)
    moved = jax.random.randint(jax.random.fold_in(own_key, 1), (pairs,), 0, 1 << 20) % (margin + 1)
    lengths = lengths.at[1:1 + 2 * pairs:2].set(giver - moved).at[2:2 + 2 * pairs:2].set(taker + moved)
    return lengths[jax.random.permutation(jax.random.fold_in(own_key, 2), number_of)]


def normal_values(key, extent, width, most, pieces=(), kind=jnp.bfloat16):
    factor_of = levels(key, extent, pieces, -0.22, 0.18) if pieces else 1.0
    values = jax.random.normal(key, extent, jnp.float32) * width * factor_of
    return jnp.minimum(jnp.maximum(values, -most), most).astype(kind)


def setup_inputs(seed: int = 0) -> dict:
    keys = jax.random.split(jax.random.key(seed), 14)
    queries = draw_queries(jax.random.fold_in(keys[13], 71), 0)
    key_rows = draw_key_rows(jax.random.fold_in(keys[13], 71), 0)
    value_rows = normal_values(keys[2], (TOKENS, KV_HEADS * HD), 1.0, 6.0, ((0, 64), (1, 4)))
    doc_ids = jnp.searchsorted(jnp.cumsum(uneven(keys[3], DOCS, TOKENS, DOC_MOST, 1)), jnp.arange(TOKENS), side="right").astype(jnp.int32)
    sink_logit = jnp.clip(3.0 + 4.0 * jax.random.uniform(keys[4], (HEADS,), jnp.float32) ** levels(keys[4], (HEADS,), ((0, 4),), -0.2, 0.2), 3.0, 7.0)
    residual = normal_values(keys[5], (TOKENS, D), 1.0, 6.0, ((0, 256),))
    out_weight = normal_values(keys[6], (HEADS * HD, D), ((HEADS * HD) ** -0.5 * 10), 3.5, ((0, 4),))
    norm_gain = jnp.clip(1.0 + 0.18 * jax.random.normal(keys[7], (D,), jnp.float32), 0.1, 1.9)
    gate_weight = normal_values(keys[8], (EXPERTS, D, FF), D ** -0.5, 0.125, ((0, 64),))
    up_weight = normal_values(keys[9], (EXPERTS, D, FF), D ** -0.5, 0.125, ((0, 64),))
    down_weight = normal_values(keys[10], (EXPERTS, FF, D), FF ** -0.5, 0.25, ((0, 64),))
    routes = draw_routes(jax.random.fold_in(keys[13], 71), 0)
    route_weights = jnp.clip(0.2 + 0.6 * jax.random.uniform(keys[12], (TOKENS, TOPK), jnp.float32) ** levels(keys[12], (TOKENS, TOPK), ((0, 256),), -0.2, 0.2), 0.2, 0.8)
    return dict(queries=queries, key_rows=key_rows, value_rows=value_rows, doc_ids=doc_ids, sink_logit=sink_logit, residual=residual, out_weight=out_weight, norm_gain=norm_gain, gate_weight=gate_weight, up_weight=up_weight, down_weight=down_weight, routes=routes, route_weights=route_weights)


neg_fill = -1e+30
eps_norm = 1e-06

def reference(queries, key_rows, value_rows, doc_ids, sink_logit, residual, out_weight, norm_gain, gate_weight, up_weight, down_weight, routes, route_weights):
    head_ratio = HEADS // KV_HEADS
    block_rows = 512
    block_total = TOKENS // block_rows
    key_pad = jnp.pad(key_rows, ((WINDOW, WINDOW), (0, 0)))
    value_pad = jnp.pad(value_rows, ((WINDOW, WINDOW), (0, 0)))
    doc_pad = jnp.pad(doc_ids, (WINDOW, WINDOW), constant_values=-1)
    sink_col = sink_logit.astype(jnp.float32).reshape(KV_HEADS, head_ratio)[:, :, None, None]

    def one_block(block_index):
        row_start = (block_index * block_rows).astype(jnp.int32)
        key_count = block_rows + 2 * WINDOW
        query_part = lax.dynamic_slice_in_dim(queries, row_start, block_rows, 0).astype(jnp.float32)
        query_part = query_part.reshape(block_rows, KV_HEADS, head_ratio, HD)
        key_part = lax.dynamic_slice_in_dim(key_pad, row_start, key_count, 0).astype(jnp.float32).reshape(key_count, KV_HEADS, HD)
        value_part = lax.dynamic_slice_in_dim(value_pad, row_start, key_count, 0).astype(jnp.float32).reshape(key_count, KV_HEADS, HD)
        query_docs = lax.dynamic_slice_in_dim(doc_ids, row_start, block_rows, 0)
        key_docs = lax.dynamic_slice_in_dim(doc_pad, row_start, key_count, 0)
        query_pos = row_start + jnp.arange(block_rows, dtype=jnp.int32)
        key_pos = row_start - WINDOW + jnp.arange(key_count, dtype=jnp.int32)
        allowed = (jnp.abs(query_pos[:, None] - key_pos[None, :]) <= WINDOW) & (query_docs[:, None] == key_docs[None, :])
        scores = jnp.einsum('qgrd,kgd->grqk', query_part, key_part) * HD ** (-0.5)
        masked = jnp.where(allowed[None, None], scores, neg_fill)
        row_top = jnp.maximum(lax.optimization_barrier(jnp.max(masked, axis=3, keepdims=True)), sink_col)
        exponent = jnp.where(allowed[None, None], jnp.exp(masked - row_top), 0.0)
        denominator = lax.optimization_barrier(jnp.sum(exponent, axis=3, keepdims=True)) + jnp.exp(sink_col - row_top)
        attn_weight = (exponent / denominator).astype(jnp.bfloat16)
        attended = jnp.einsum('grqk,kgd->qgrd', attn_weight.astype(jnp.float32), value_part)
        return attended.astype(jnp.bfloat16).reshape(block_rows, HEADS * HD)
    attended = lax.map(one_block, jnp.arange(block_total, dtype=jnp.int32)).reshape(TOKENS, HEADS * HD)
    group_cols = HEADS * HD // N_TP
    summed = jnp.zeros((TOKENS, D), jnp.float32)
    for group_index in range(N_TP):
        cols = attended[:, group_index * group_cols:(group_index + 1) * group_cols]
        rows_w = out_weight[group_index * group_cols:(group_index + 1) * group_cols]
        partial_value = jnp.dot(cols, rows_w, preferred_element_type=jnp.float32).astype(jnp.bfloat16)
        partial_value = lax.optimization_barrier(partial_value)
        summed = summed + partial_value.astype(jnp.float32)
    stream = (residual.astype(jnp.float32) + summed).astype(jnp.bfloat16)
    stream_f = stream.astype(jnp.float32)
    scale = lax.rsqrt(lax.optimization_barrier(jnp.mean(stream_f * stream_f, axis=1, keepdims=True)) + eps_norm)
    normed = (stream_f * scale * norm_gain.astype(jnp.float32)[None, :]).astype(jnp.bfloat16)
    flat_routes = routes.reshape(-1)
    flat_weights = route_weights.reshape(-1).astype(jnp.float32)
    per_expert = TOKENS * TOPK // EXPERTS

    def expert_step(accum, inputs):
        expert_id, gate_one, up_one, down_one = inputs
        found = jnp.nonzero(flat_routes == expert_id, size=per_expert)[0].astype(jnp.int32)
        token_index = found // TOPK
        rows = normed[token_index]
        gate_act = jnp.dot(rows, gate_one, preferred_element_type=jnp.float32)
        up_act = jnp.dot(rows, up_one, preferred_element_type=jnp.float32)
        hidden = (jax.nn.silu(gate_act) * up_act).astype(jnp.bfloat16)
        expert_out = jnp.dot(hidden, down_one, preferred_element_type=jnp.float32).astype(jnp.bfloat16)
        accum = accum.at[token_index].add(flat_weights[found][:, None] * expert_out.astype(jnp.float32))
        return (accum, None)
    accum0 = jnp.zeros((TOKENS, D), jnp.float32)
    accum, _ = lax.scan(expert_step, accum0, (jnp.arange(EXPERTS, dtype=jnp.int32), gate_weight, up_weight, down_weight))
    return (stream_f + accum).astype(jnp.bfloat16)
```

```python
import jax
import jax.numpy as jnp
from jax import lax
from jax.experimental import pallas as pl
from jax.experimental.pallas import tpu as pltpu
from jax.sharding import PartitionSpec as P

HD = 64
WINDOW = 128
NEG = -1e30
EPS = 1e-06
F32 = jnp.float32
BF16 = jnp.bfloat16
NT = (((1,), (1,)), ((), ()))
TN = (((0,), (0,)), ((), ()))
VMEM = pl.BlockSpec(memory_space=pltpu.VMEM)


def pack_body(k_ref, v_ref, doc_ref, low_ref, high_ref):
    rows = k_ref.shape[0]
    docs = (doc_ref[...] + 1).astype(F32)
    last = docs.shape[0] - 1
    for ref, start, row in ((low_ref, 0, 0), (high_ref, rows - WINDOW, last)):
        ref[0:WINDOW, 0:128] = k_ref[start : start + WINDOW, :]
        ref[0:WINDOW, 128:256] = v_ref[start : start + WINDOW, :]
        line = jnp.broadcast_to(docs[row : row + 1, :], (16, 128)).astype(BF16)
        ref[WINDOW : WINDOW + 16, 0:128] = line
        ref[WINDOW : WINDOW + 16, 128:256] = line


def slots_body(routes_ref, slots_ref, *, experts, capacity):
    rows = routes_ref.shape[1]
    first = routes_ref[0:1, :]
    second = routes_ref[1:2, :]
    ids = lax.broadcasted_iota(jnp.int32, (experts, rows), 0)
    named = jnp.where((ids == first) | (ids == second), 1.0, 0.0)
    before = lax.broadcasted_iota(jnp.int32, (rows, rows), 0) < lax.broadcasted_iota(
        jnp.int32, (rows, rows), 1
    )
    earlier = jnp.dot(
        named.astype(BF16),
        jnp.where(before, 1.0, 0.0).astype(BF16),
        preferred_element_type=F32,
    )
    for k, route in ((0, first), (1, second)):
        rank = jnp.sum(jnp.where(ids == route, earlier, 0.0), axis=0, keepdims=True)
        slots_ref[k : k + 1, :] = route * capacity + rank.astype(jnp.int32)


def attend_body(q_ref, k_ref, v_ref, doc_ref, low_ref, high_ref, sink_ref, out_ref, kvar, vt, kdoc):
    block = pl.program_id(0)
    rows = k_ref.shape[0]

    @pl.when(block == 0)
    def _():
        lane = lax.broadcasted_iota(jnp.int32, (WINDOW, 128), 1)
        count = rows // WINDOW + 2
        for part in range(count):
            here = slice(part * WINDOW, (part + 1) * WINDOW)
            if part == 0:
                keys = low_ref[0:WINDOW, 0:128]
                values = low_ref[0:WINDOW, 128:256]
                docs = low_ref[WINDOW : WINDOW + 1, 0:128].astype(F32)
            elif part == count - 1:
                keys = high_ref[0:WINDOW, 0:128]
                values = high_ref[0:WINDOW, 128:256]
                docs = high_ref[WINDOW : WINDOW + 1, 0:128].astype(F32)
            else:
                keys = k_ref[(part - 1) * WINDOW : part * WINDOW, :]
                values = v_ref[(part - 1) * WINDOW : part * WINDOW, :]
                docs = (doc_ref[part - 1 : part, :] + 1).astype(F32)
            scaled = keys.astype(F32) * HD ** (-0.5)
            turned = pltpu.roll(scaled, 64, 1)
            left = lane < 64
            kvar[0, here, :] = jnp.where(left, scaled, 0.0).astype(BF16)
            kvar[1, here, :] = jnp.where(left, 0.0, turned).astype(BF16)
            kvar[2, here, :] = jnp.where(left, turned, 0.0).astype(BF16)
            kvar[3, here, :] = jnp.where(left, 0.0, scaled).astype(BF16)
            vt[:, here] = values.T
            kdoc[here, :] = jnp.broadcast_to(docs, (WINDOW, 128)).T

    start = pl.multiple_of(block * WINDOW, WINDOW)
    span = 3 * WINDOW
    query_docs = (doc_ref[pl.ds(block, 1), :] + 1).astype(F32)
    ahead = lax.broadcasted_iota(jnp.int32, (span, WINDOW), 0) - lax.broadcasted_iota(
        jnp.int32, (span, WINDOW), 1
    )
    allowed = (ahead >= 0) & (ahead <= 2 * WINDOW) & (kdoc[pl.ds(start, span), :] == query_docs)
    bias = jnp.where(allowed, 0.0, NEG)
    groups = k_ref.shape[1] // HD
    ratio = q_ref.shape[1] // k_ref.shape[1]
    for pair in range(groups * ratio // 2):
        group = pair // (ratio // 2)
        queries = q_ref[:, pair * 128 : (pair + 1) * 128]
        halves = []
        for half in range(2):
            head = pair * 2 + half
            scores = lax.dot_general(
                kvar[group * 2 + half, pl.ds(start, span), :],
                queries,
                NT,
                preferred_element_type=F32,
            )
            scores = scores + bias
            sink = sink_ref[head]
            top = jnp.maximum(jnp.max(scores, axis=0, keepdims=True), sink)
            weight = jnp.exp(scores - top)
            total = jnp.sum(weight, axis=0, keepdims=True) + jnp.exp(sink - top)
            halves.append((weight * (1.0 / total)).astype(BF16))
        both = jnp.concatenate(halves, axis=1)
        mixed = jnp.dot(
            vt[group * HD : (group + 1) * HD, pl.ds(start, span)],
            both,
            preferred_element_type=F32,
        )
        stacked = jnp.concatenate([mixed[:, 0:128], mixed[:, 128:256]], axis=0)
        out_ref[:, pair * 128 : (pair + 1) * 128] = stacked.T.astype(BF16)


def project_body(
    core_ref,
    here_att,
    there_att,
    here_w,
    there_w,
    residual_ref,
    gain_ref,
    slots_ref,
    out_ref,
    stream_ref,
    acc,
):
    step = pl.program_id(0)
    partial = jnp.dot(here_att[0], here_w[0], preferred_element_type=F32) + jnp.dot(
        there_att[0], there_w[0], preferred_element_type=F32
    )
    partial = partial.astype(BF16).astype(F32)

    @pl.when(step == 0)
    def _():
        acc[...] = partial

    @pl.when(step > 0)
    def _():
        acc[...] += partial

    @pl.when(step == pl.num_programs(0) - 1)
    def _():
        stream = (residual_ref[...].astype(F32) + acc[...]).astype(BF16)
        stream_ref[...] = stream
        wide = stream.astype(F32)
        scale = lax.rsqrt(jnp.mean(wide * wide, axis=1, keepdims=True) + EPS)
        normed = (wide * scale * gain_ref[...]).astype(BF16)
        ids = lax.broadcasted_iota(jnp.int32, (out_ref.shape[0], slots_ref.shape[1]), 0)
        place = (ids == slots_ref[0:1, :]) | (ids == slots_ref[1:2, :])
        out_ref[...] = jnp.dot(
            jnp.where(place, 1.0, 0.0).astype(BF16), normed, preferred_element_type=F32
        ).astype(BF16)


def expert_body(x_ref, gate_ref, up_ref, down_ref, out_ref, acc):
    step = pl.program_id(0)
    gate_act = jnp.dot(x_ref[...], gate_ref[0], preferred_element_type=F32)
    up_act = jnp.dot(x_ref[...], up_ref[0], preferred_element_type=F32)
    hidden = (gate_act / (1.0 + jnp.exp(-gate_act)) * up_act).astype(BF16)
    part = jnp.dot(hidden, down_ref[0], preferred_element_type=F32)
    last = pl.num_programs(0) - 1

    @pl.when(step == 0)
    def _():
        acc[...] = part

    @pl.when((step > 0) & (step < last))
    def _():
        acc[...] += part

    @pl.when(step == last)
    def _():
        out_ref[...] = (acc[...] + part).astype(BF16)


def combine_body(back_ref, stream_ref, slots_ref, weights_ref, out_ref):
    rows = stream_ref.shape[0]
    slots = back_ref.shape[0]
    width = stream_ref.shape[1]
    ids = lax.broadcasted_iota(jnp.int32, (slots, rows), 0)
    total = None
    for k in range(2):
        pick = jnp.where(ids == slots_ref[k : k + 1, :], 1.0, 0.0).astype(BF16)
        chosen = lax.dot_general(pick, back_ref[...], TN, preferred_element_type=F32)
        line = weights_ref[k : k + 1, :]
        columns = [
            jnp.broadcast_to(line[:, i : i + 128], (128, 128)).T for i in range(0, rows, 128)
        ]
        factor = jnp.concatenate(columns, axis=0)
        factor = jnp.concatenate([factor] * (width // 128), axis=1)
        term = factor * chosen
        total = term if total is None else total + term
    out_ref[...] = (stream_ref[...].astype(F32) + total).astype(BF16)


def per_device(
    queries,
    key_rows,
    value_rows,
    doc_ids,
    sink_logit,
    residual,
    out_weight,
    norm_gain,
    gate_weight,
    up_weight,
    down_weight,
    routes,
    route_weights,
):
    local_rows = queries.shape[0]
    home_rows, width = residual.shape
    devices = lax.axis_size("sp")
    ways = lax.axis_size("tp")
    experts = devices * gate_weight.shape[0]
    route_count = routes.shape[1]
    capacity = route_count * home_rows // experts
    slot_count = experts * capacity
    shard = out_weight.shape[0]
    core = lax.axis_index("sp") % 2
    half_weight = lax.dynamic_slice_in_dim(out_weight, core * (shard // 2), shard // 2, 0)
    here_weight = lax.all_gather(half_weight, "tp", axis=0)

    doc_lines = doc_ids.reshape(local_rows // 128, 128)
    halo = jax.ShapeDtypeStruct((WINDOW + 16, 256), BF16)
    first_rows, last_rows = pl.pallas_call(
        pack_body,
        out_shape=(halo, halo),
        in_specs=[VMEM] * 3,
        out_specs=(VMEM, VMEM),
        name="pack",
    )(key_rows, value_rows, doc_lines)
    forward = [(i, i + 1) for i in range(devices - 1)]
    backward = [(j, i) for i, j in forward]
    low = lax.ppermute(last_rows, "sp", forward)
    high = lax.ppermute(first_rows, "sp", backward)

    slots = pl.pallas_call(
        lambda r, s: slots_body(r, s, experts=experts, capacity=capacity),
        out_shape=jax.ShapeDtypeStruct((route_count, home_rows), jnp.int32),
        in_specs=[VMEM],
        out_specs=VMEM,
        name="slots",
    )(routes.T)

    blocks = local_rows // WINDOW
    whole = lambda shape: pl.BlockSpec(shape, lambda i: (0,) * len(shape))
    attended = pl.pallas_call(
        attend_body,
        grid=(blocks,),
        out_shape=jax.ShapeDtypeStruct(queries.shape, BF16),
        in_specs=[
            pl.BlockSpec((WINDOW, queries.shape[1]), lambda i: (i, 0)),
            whole(key_rows.shape),
            whole(value_rows.shape),
            whole(doc_lines.shape),
            whole(halo.shape),
            whole(halo.shape),
            pl.BlockSpec(memory_space=pltpu.SMEM),
        ],
        out_specs=pl.BlockSpec((WINDOW, queries.shape[1]), lambda i: (i, 0)),
        scratch_shapes=[
            pltpu.VMEM((4, local_rows + 2 * WINDOW, 128), BF16),
            pltpu.VMEM((128, local_rows + 2 * WINDOW), BF16),
            pltpu.VMEM((local_rows + 2 * WINDOW, 128), F32),
        ],
        name="attend",
    )(queries, key_rows, value_rows, doc_lines, low, high, sink_logit)

    columns = queries.shape[1]
    regrouped = lax.all_to_all(
        attended.reshape(ways, home_rows, columns), "tp", split_axis=0, concat_axis=0, tiled=True
    )
    swap = [(i, i ^ 1) for i in range(devices)]
    there_weight = lax.ppermute(here_weight, "sp", swap)

    fixed = lambda shape: pl.BlockSpec(shape, lambda i, c: (0,) * len(shape))
    outgoing, stream = pl.pallas_call(
        project_body,
        grid_spec=pltpu.PrefetchScalarGridSpec(
            num_scalar_prefetch=1,
            grid=(ways,),
            in_specs=[
                pl.BlockSpec((1, home_rows, columns // 2), lambda i, c: (i, 0, c[0])),
                pl.BlockSpec((1, home_rows, columns // 2), lambda i, c: (i, 0, 1 - c[0])),
                pl.BlockSpec((1, shard // 2, width), lambda i, c: (i, 0, 0)),
                pl.BlockSpec((1, shard // 2, width), lambda i, c: (i, 0, 0)),
                fixed((home_rows, width)),
                fixed((1, width)),
                fixed((route_count, home_rows)),
            ],
            out_specs=[fixed((slot_count, width)), fixed((home_rows, width))],
            scratch_shapes=[pltpu.VMEM((home_rows, width), F32)],
        ),
        out_shape=(
            jax.ShapeDtypeStruct((slot_count, width), BF16),
            jax.ShapeDtypeStruct((home_rows, width), BF16),
        ),
        name="project",
    )(
        core.astype(jnp.int32).reshape(1),
        regrouped,
        regrouped,
        here_weight,
        there_weight,
        residual,
        norm_gain.reshape(1, width),
        slots,
    )

    incoming = lax.all_to_all(
        outgoing.reshape(devices, -1, width), "sp", split_axis=0, concat_axis=0, tiled=True
    )
    hidden_units = gate_weight.shape[2]
    pieces = 2
    piece = hidden_units // pieces
    produced = pl.pallas_call(
        expert_body,
        grid=(pieces,),
        out_shape=jax.ShapeDtypeStruct((slot_count, width), BF16),
        in_specs=[
            whole((slot_count, width)),
            pl.BlockSpec((1, width, piece), lambda i: (0, 0, i)),
            pl.BlockSpec((1, width, piece), lambda i: (0, 0, i)),
            pl.BlockSpec((1, piece, width), lambda i: (0, i, 0)),
        ],
        out_specs=whole((slot_count, width)),
        scratch_shapes=[pltpu.VMEM((slot_count, width), F32)],
        name="experts",
    )(incoming.reshape(slot_count, width), gate_weight, up_weight, down_weight)
    returned = lax.all_to_all(
        produced.reshape(devices, -1, width), "sp", split_axis=0, concat_axis=0, tiled=True
    )
    half = width // 2
    return pl.pallas_call(
        combine_body,
        grid=(2,),
        out_shape=jax.ShapeDtypeStruct((home_rows, width), BF16),
        in_specs=[
            pl.BlockSpec((slot_count, half), lambda i: (0, i)),
            pl.BlockSpec((home_rows, half), lambda i: (0, i)),
            whole((route_count, home_rows)),
            whole((route_count, home_rows)),
        ],
        out_specs=pl.BlockSpec((home_rows, half), lambda i: (0, i)),
        name="combine",
    )(returned.reshape(slot_count, width), stream, slots, route_weights.T)


def solution(mesh):
    return jax.shard_map(
        per_device,
        mesh=mesh,
        in_specs=(
            P("sp", "tp"),
            P("sp", "tp"),
            P("sp", "tp"),
            P("sp"),
            P("tp"),
            P(("sp", "tp"), None),
            P("tp", None),
            P(),
            P("sp", None, None),
            P("sp", None, None),
            P("sp", None, None),
            P(("sp", "tp"), None),
            P(("sp", "tp"), None),
        ),
        out_specs=P(("sp", "tp"), None),
        check_vma=False,
    )
```

```python
from functools import partial

import jax
import jax.numpy as jnp
from jax import lax
from jax.experimental import pallas as pl
from jax.experimental.pallas import tpu as pltpu
from jax.sharding import PartitionSpec as P


HD = 64
WINDOW = 128
NEG = -1e30
EPS = 1e-06
F32 = jnp.float32
BF16 = jnp.bfloat16
NT = (((1,), (1,)), ((), ()))
TN = (((0,), (0,)), ((), ()))
VMEM = pl.BlockSpec(memory_space=pltpu.VMEM)


def pack_body(k_ref, v_ref, doc_ref, low_ref, high_ref):
    rows = k_ref.shape[0]
    docs = (doc_ref[...] + 1).astype(F32)
    last = docs.shape[0] - 1
    for ref, start, row in ((low_ref, 0, 0), (high_ref, rows - WINDOW, last)):
        ref[0:WINDOW, 0:128] = k_ref[start : start + WINDOW, :]
        ref[0:WINDOW, 128:256] = v_ref[start : start + WINDOW, :]
        line = jnp.broadcast_to(docs[row : row + 1, :], (16, 128)).astype(BF16)
        ref[WINDOW : WINDOW + 16, 0:128] = line
        ref[WINDOW : WINDOW + 16, 128:256] = line


def exclusive_count(named):
    rows = named.shape[1]
    before = lax.broadcasted_iota(jnp.int32, (rows, rows), 0) < lax.broadcasted_iota(
        jnp.int32, (rows, rows), 1
    )
    return jnp.dot(
        named.astype(BF16), jnp.where(before, 1.0, 0.0).astype(BF16), preferred_element_type=F32
    )


def group_place(route, groups, group_size):
    rows = route.shape[1]
    ids = lax.broadcasted_iota(jnp.int32, (8, rows), 0)
    group = route // group_size
    inside = ids == group
    earlier = exclusive_count(jnp.where(inside, 1.0, 0.0))
    rank = jnp.sum(jnp.where(inside, earlier, 0.0), axis=0, keepdims=True).astype(jnp.int32)
    place = group * (rows // groups) + rank
    return jnp.where(lax.broadcasted_iota(jnp.int32, (rows, rows), 0) == place, 1.0, 0.0).astype(BF16)


def sort_body(routes_ref, weights_ref, residual_ref, out_ref, *, experts, groups, capacity):
    rows = routes_ref.shape[1]
    width = residual_ref.shape[1]
    group_size = experts // groups
    first = routes_ref[0:1, :]
    second = routes_ref[1:2, :]
    ids = lax.broadcasted_iota(jnp.int32, (experts, rows), 0)
    earlier = exclusive_count(jnp.where((ids == first) | (ids == second), 1.0, 0.0))
    facts = []
    for route in (first, second):
        rank = jnp.sum(jnp.where(ids == route, earlier, 0.0), axis=0, keepdims=True)
        facts.append((route % group_size * capacity).astype(F32) + rank)
    for k in range(2):
        left = weights_ref[k : k + 1, :]
        for _ in range(3):
            part = left.astype(BF16).astype(F32)
            facts.append(part)
            left = left - part
    row_of = lax.broadcasted_iota(jnp.int32, (128, rows), 0)
    table = jnp.zeros((128, rows), F32)
    for i, fact in enumerate(facts):
        table = jnp.where(row_of == i, fact, table)
    order = group_place(first, groups, group_size)
    out_ref[:, 0:width] = jnp.dot(order, residual_ref[...], preferred_element_type=F32).astype(BF16)
    out_ref[:, width:] = lax.dot_general(
        order, table.astype(BF16), NT, preferred_element_type=F32
    ).astype(BF16)


def attend_body(
    q_ref, k_ref, v_ref, doc_ref, low_ref, high_ref, sink_ref, routes_ref, out_ref, kvar, vt, kdoc, buf, *, groups_all, group_size
):
    block = pl.program_id(0)
    rows = k_ref.shape[0]

    @pl.when(block == 0)
    def _():
        lane = lax.broadcasted_iota(jnp.int32, (WINDOW, 128), 1)
        count = rows // WINDOW + 2
        for part in range(count):
            here = slice(part * WINDOW, (part + 1) * WINDOW)
            if part == 0:
                keys = low_ref[0:WINDOW, 0:128]
                values = low_ref[0:WINDOW, 128:256]
                docs = low_ref[WINDOW : WINDOW + 1, 0:128].astype(F32)
            elif part == count - 1:
                keys = high_ref[0:WINDOW, 0:128]
                values = high_ref[0:WINDOW, 128:256]
                docs = high_ref[WINDOW : WINDOW + 1, 0:128].astype(F32)
            else:
                keys = k_ref[(part - 1) * WINDOW : part * WINDOW, :]
                values = v_ref[(part - 1) * WINDOW : part * WINDOW, :]
                docs = (doc_ref[part - 1 : part, :] + 1).astype(F32)
            scaled = keys.astype(F32) * HD ** (-0.5)
            turned = pltpu.roll(scaled, 64, 1)
            left = lane < 64
            kvar[0, here, :] = jnp.where(left, scaled, 0.0).astype(BF16)
            kvar[1, here, :] = jnp.where(left, 0.0, turned).astype(BF16)
            kvar[2, here, :] = jnp.where(left, turned, 0.0).astype(BF16)
            kvar[3, here, :] = jnp.where(left, 0.0, scaled).astype(BF16)
            vt[:, here] = values.T
            kdoc[here, :] = jnp.broadcast_to(docs, (WINDOW, 128)).T

    subs = q_ref.shape[0] // WINDOW
    for sub in range(subs):
        start = pl.multiple_of((block * subs + sub) * WINDOW, WINDOW)
        span = 3 * WINDOW
        query_docs = (doc_ref[pl.ds(block * subs + sub, 1), :] + 1).astype(F32)
        ahead = lax.broadcasted_iota(jnp.int32, (span, WINDOW), 0) - lax.broadcasted_iota(
            jnp.int32, (span, WINDOW), 1
        )
        allowed = (ahead >= 0) & (ahead <= 2 * WINDOW) & (kdoc[pl.ds(start, span), :] == query_docs)
        bias = jnp.where(allowed, 0.0, NEG)
        groups = k_ref.shape[1] // HD
        ratio = q_ref.shape[1] // k_ref.shape[1]
        for pair in range(groups * ratio // 2):
            group = pair // (ratio // 2)
            queries = q_ref[sub * WINDOW : (sub + 1) * WINDOW, pair * 128 : (pair + 1) * 128]
            halves = []
            for half in range(2):
                head = pair * 2 + half
                scores = lax.dot_general(
                    kvar[group * 2 + half, pl.ds(start, span), :],
                    queries,
                    NT,
                    preferred_element_type=F32,
                )
                scores = scores + bias
                sink = sink_ref[head]
                top = jnp.maximum(jnp.max(scores, axis=0, keepdims=True), sink)
                weight = jnp.exp(scores - top)
                total = jnp.sum(weight, axis=0, keepdims=True) + jnp.exp(sink - top)
                halves.append((weight * (1.0 / total)).astype(BF16))
            both = jnp.concatenate(halves, axis=1)
            mixed = jnp.dot(
                vt[group * HD : (group + 1) * HD, pl.ds(start, span)],
                both,
                preferred_element_type=F32,
            )
            stacked = jnp.concatenate([mixed[:, 0:128], mixed[:, 128:256]], axis=0)
            buf[sub * WINDOW : (sub + 1) * WINDOW, pair * 128 : (pair + 1) * 128] = stacked.T.astype(BF16)
    order = group_place(routes_ref[0, 0:1, :], groups_all, group_size)
    out_ref[...] = (
        jnp.dot(order, buf[...], preferred_element_type=F32).astype(BF16).reshape(out_ref.shape)
    )


def relay_slots(facts, k, capacity):
    rows = facts.shape[0]
    blocks = 4
    fact = facts[:, k : k + 1].astype(F32).astype(jnp.int32)
    source = lax.broadcasted_iota(jnp.int32, (rows, 1), 0) // (rows // blocks)
    return fact // capacity * (capacity * blocks) + source * capacity + fact % capacity


def project_body(
    place_ref,
    here_att,
    there_att,
    here_w,
    there_w,
    own_ref,
    hop1_ref,
    hop2_ref,
    hop3_ref,
    gain_ref,
    out_ref,
    stream_ref,
    facts_ref,
    acc,
    residual_ref,
    *,
    capacity,
):
    step = pl.program_id(0)
    rows, width = stream_ref.shape
    here = here_att[...].reshape(rows, here_att.shape[3])
    there = there_att[...].reshape(rows, there_att.shape[3])
    share = jnp.dot(here, here_w[0], preferred_element_type=F32) + jnp.dot(
        there, there_w[0], preferred_element_type=F32
    )
    share = share.astype(BF16).astype(F32)

    @pl.when(step == 0)
    def _():
        acc[...] = share
        blocks = 4
        size = rows // blocks
        for hop, ref in enumerate((own_ref.at[0], hop1_ref, hop2_ref, hop3_ref)):
            source = (place_ref[1] + blocks - hop) % blocks
            residual_ref[pl.ds(pl.multiple_of(source * size, size), size), :] = ref[...]

    @pl.when(step > 0)
    def _():
        acc[...] += share

    @pl.when(step == pl.num_programs(0) - 1)
    def _():
        stream = (residual_ref[:, 0:width].astype(F32) + acc[...]).astype(BF16)
        stream_ref[...] = stream
        wide = stream.astype(F32)
        scale = lax.rsqrt(jnp.mean(wide * wide, axis=1, keepdims=True) + EPS)
        normed = (wide * scale * gain_ref[...]).astype(BF16)
        facts = residual_ref[:, width:]
        facts_ref[...] = facts
        ids = lax.broadcasted_iota(jnp.int32, (rows, out_ref.shape[0]), 1)
        place = (ids == relay_slots(facts, 0, capacity)) | (ids == relay_slots(facts, 1, capacity))
        out_ref[...] = lax.dot_general(
            jnp.where(place, 1.0, 0.0).astype(BF16), normed, TN, preferred_element_type=F32
        ).astype(BF16)


def expert_body(x_ref, gate_ref, up_ref, down_ref, out_ref, acc):
    step = pl.program_id(0)
    gate_act = jnp.dot(x_ref[...], gate_ref[0], preferred_element_type=F32)
    up_act = jnp.dot(x_ref[...], up_ref[0], preferred_element_type=F32)
    hidden = (gate_act / (1.0 + jnp.exp(-gate_act)) * up_act).astype(BF16)
    part = jnp.dot(hidden, down_ref[0], preferred_element_type=F32)
    last = pl.num_programs(0) - 1

    @pl.when(step == 0)
    def _():
        acc[...] = part

    @pl.when((step > 0) & (step < last))
    def _():
        acc[...] += part

    @pl.when(step == last)
    def _():
        out_ref[...] = (acc[...] + part).astype(BF16)


def combine_body(back_ref, stream_ref, facts_ref, out_ref, *, capacity):
    facts = facts_ref[...]
    rows = stream_ref.shape[0]
    ids = lax.broadcasted_iota(jnp.int32, (rows, back_ref.shape[0]), 1)
    total = None
    for k in range(2):
        pick = jnp.where(ids == relay_slots(facts, k, capacity), 1.0, 0.0).astype(BF16)
        chosen = jnp.dot(pick, back_ref[...], preferred_element_type=F32)
        parts = facts[:, 2 + 3 * k : 5 + 3 * k].astype(F32)
        factor = parts[:, 0:1] + parts[:, 1:2] + parts[:, 2:3]
        term = factor * chosen
        total = term if total is None else total + term
    out_ref[...] = (stream_ref[...].astype(F32) + total).astype(BF16)


def home_body(rows_ref, routes_ref, out_ref, *, groups, group_size):
    order = group_place(routes_ref[0:1, :], groups, group_size)
    out_ref[...] = lax.dot_general(order, rows_ref[...], TN, preferred_element_type=F32).astype(BF16)


def per_device(
    queries,
    key_rows,
    value_rows,
    doc_ids,
    sink_logit,
    residual,
    out_weight,
    norm_gain,
    gate_weight,
    up_weight,
    down_weight,
    routes,
    route_weights,
):
    local_rows = queries.shape[0]
    home_rows, width = residual.shape
    devices = lax.axis_size("sp")
    ways = lax.axis_size("tp")
    experts = devices * gate_weight.shape[0]
    route_count = routes.shape[1]
    capacity = route_count * home_rows // experts
    slot_count = experts * capacity
    shard = out_weight.shape[0]
    core = lax.axis_index("sp") % 2
    half_weight = lax.dynamic_slice_in_dim(out_weight, core * (shard // 2), shard // 2, 0)
    here_weight = lax.all_gather(half_weight, "tp", axis=0)

    doc_lines = doc_ids.reshape(local_rows // 128, 128)
    halo = jax.ShapeDtypeStruct((WINDOW + 16, 256), BF16)
    first_rows, last_rows = pl.pallas_call(
        pack_body,
        out_shape=(halo, halo),
        in_specs=[VMEM] * 3,
        out_specs=(VMEM, VMEM),
        name="pack",
    )(key_rows, value_rows, doc_lines)
    forward = [(i, i + 1) for i in range(devices - 1)]
    backward = [(j, i) for i, j in forward]
    low = lax.ppermute(last_rows, "sp", forward)
    high = lax.ppermute(first_rows, "sp", backward)

    groups = 4
    group_size = experts // groups
    inner = devices // groups
    same_place = [[g * inner + r for g in range(groups)] for r in range(inner)]
    same_group = [[g * inner + r for r in range(inner)] for g in range(groups)]
    relays = [
        [(g * inner + r) * ways + y for g in range(groups) for y in range(ways)] for r in range(inner)
    ]
    route_lines = routes.T
    weight_lines = route_weights.T
    all_routes = lax.all_gather(route_lines, "tp", axis=0)
    facts_width = 128
    payload = pl.pallas_call(
        partial(sort_body, experts=experts, groups=groups, capacity=capacity),
        out_shape=jax.ShapeDtypeStruct((home_rows, width + facts_width), BF16),
        in_specs=[VMEM] * 3,
        out_specs=VMEM,
        name="sort",
    )(route_lines, weight_lines, residual)
    own_group = lax.axis_index("sp") // inner
    sorted_rows = payload.reshape(groups, home_rows // groups, width + facts_width)
    hops = []
    for hop in range(1, groups):
        moved = [(i, (i + hop * inner) % devices) for i in range(devices)]
        chunk = lax.dynamic_index_in_dim(sorted_rows, (own_group + hop) % groups, 0, False)
        hops.append(lax.ppermute(chunk, "sp", moved))

    columns = queries.shape[1]
    group_rows = home_rows // groups
    whole = lambda shape: pl.BlockSpec(shape, lambda i: (0,) * len(shape))
    attend = pl.pallas_call(
        partial(attend_body, groups_all=groups, group_size=group_size),
        grid=(ways,),
        out_shape=jax.ShapeDtypeStruct((groups, ways, group_rows, columns), BF16),
        in_specs=[
            pl.BlockSpec((home_rows, columns), lambda i: (i, 0)),
            whole(key_rows.shape),
            whole(value_rows.shape),
            whole(doc_lines.shape),
            whole(halo.shape),
            whole(halo.shape),
            pl.BlockSpec(memory_space=pltpu.SMEM),
            pl.BlockSpec((1, route_count, home_rows), lambda i: (i, 0, 0)),
        ],
        out_specs=pl.BlockSpec((groups, 1, group_rows, columns), lambda i: (0, i, 0, 0)),
        scratch_shapes=[
            pltpu.VMEM((4, local_rows + 2 * WINDOW, 128), BF16),
            pltpu.VMEM((128, local_rows + 2 * WINDOW), BF16),
            pltpu.VMEM((local_rows + 2 * WINDOW, 128), F32),
            pltpu.VMEM((home_rows, columns), BF16),
        ],
        name="attend",
    )
    attended = attend(queries, key_rows, value_rows, doc_lines, low, high, sink_logit, all_routes)

    pieces = lax.all_to_all(
        attended.reshape(groups * ways, group_rows, columns),
        ("sp", "tp"),
        split_axis=0,
        concat_axis=0,
        tiled=True,
        axis_index_groups=relays,
    ).reshape(groups, ways, group_rows, columns)
    swap = [(i, i ^ 1) for i in range(devices)]
    late_weight, pieces = lax.optimization_barrier((here_weight, pieces))
    there_weight = lax.ppermute(late_weight, "sp", swap)

    fixed = lambda shape: pl.BlockSpec(shape, lambda i, c: (0,) * len(shape))
    outgoing, stream, facts = pl.pallas_call(
        partial(project_body, capacity=capacity),
        grid_spec=pltpu.PrefetchScalarGridSpec(
            num_scalar_prefetch=1,
            grid=(ways,),
            in_specs=[
                pl.BlockSpec((groups, 1, group_rows, columns // 2), lambda i, c: (0, i, 0, c[0])),
                pl.BlockSpec((groups, 1, group_rows, columns // 2), lambda i, c: (0, i, 0, 1 - c[0])),
                pl.BlockSpec((1, shard // 2, width), lambda i, c: (i, 0, 0)),
                pl.BlockSpec((1, shard // 2, width), lambda i, c: (i, 0, 0)),
                pl.BlockSpec((1, group_rows, width + facts_width), lambda i, c: (c[1], 0, 0)),
                fixed((group_rows, width + facts_width)),
                fixed((group_rows, width + facts_width)),
                fixed((group_rows, width + facts_width)),
                fixed((1, width)),
            ],
            out_specs=[
                fixed((slot_count, width)),
                fixed((home_rows, width)),
                fixed((home_rows, facts_width)),
            ],
            scratch_shapes=[
                pltpu.VMEM((home_rows, width), F32),
                pltpu.VMEM((home_rows, width + facts_width), BF16),
            ],
        ),
        out_shape=(
            jax.ShapeDtypeStruct((slot_count, width), BF16),
            jax.ShapeDtypeStruct((home_rows, width), BF16),
            jax.ShapeDtypeStruct((home_rows, facts_width), BF16),
        ),
        name="project",
    )(
        jnp.stack([core, own_group]).astype(jnp.int32),
        pieces,
        pieces,
        late_weight,
        there_weight,
        sorted_rows,
        *hops,
        norm_gain.reshape(1, width),
    )

    inside = lambda x: lax.all_to_all(
        x.reshape(inner, -1, width),
        "sp",
        split_axis=0,
        concat_axis=0,
        tiled=True,
        axis_index_groups=same_group,
    ).reshape(slot_count, width)
    incoming = inside(outgoing)
    hidden_units = gate_weight.shape[2]
    cuts = 2
    cut = hidden_units // cuts
    produced = pl.pallas_call(
        expert_body,
        grid=(cuts,),
        out_shape=jax.ShapeDtypeStruct((slot_count, width), BF16),
        in_specs=[
            whole((slot_count, width)),
            pl.BlockSpec((1, width, cut), lambda i: (0, 0, i)),
            pl.BlockSpec((1, width, cut), lambda i: (0, 0, i)),
            pl.BlockSpec((1, cut, width), lambda i: (0, i, 0)),
        ],
        out_specs=whole((slot_count, width)),
        scratch_shapes=[pltpu.VMEM((slot_count, width), F32)],
        name="experts",
    )(incoming, gate_weight, up_weight, down_weight)
    returned = inside(produced)
    half = width // 2
    finished = pl.pallas_call(
        partial(combine_body, capacity=capacity),
        grid=(2,),
        out_shape=jax.ShapeDtypeStruct((home_rows, width), BF16),
        in_specs=[
            pl.BlockSpec((slot_count, half), lambda i: (0, i)),
            pl.BlockSpec((home_rows, half), lambda i: (0, i)),
            whole((home_rows, facts_width)),
        ],
        out_specs=pl.BlockSpec((home_rows, half), lambda i: (0, i)),
        name="combine",
    )(returned, stream, facts)
    home = lax.all_to_all(
        finished.reshape(groups, group_rows, width),
        "sp",
        split_axis=0,
        concat_axis=0,
        tiled=True,
        axis_index_groups=same_place,
    ).reshape(home_rows, width)
    return pl.pallas_call(
        partial(home_body, groups=groups, group_size=group_size),
        grid=(2,),
        out_shape=jax.ShapeDtypeStruct((home_rows, width), BF16),
        in_specs=[pl.BlockSpec((home_rows, half), lambda i: (0, i)), whole((route_count, home_rows))],
        out_specs=pl.BlockSpec((home_rows, half), lambda i: (0, i)),
        name="home",
    )(home, route_lines)


def solution(mesh):
    return jax.shard_map(
        per_device,
        mesh=mesh,
        in_specs=(
            P("sp", "tp"),
            P("sp", "tp"),
            P("sp", "tp"),
            P("sp"),
            P("tp"),
            P(("sp", "tp"), None),
            P("tp", None),
            P(),
            P("sp", None, None),
            P("sp", None, None),
            P("sp", None, None),
            P(("sp", "tp"), None),
            P(("sp", "tp"), None),
        ),
        out_specs=P(("sp", "tp"), None),
        check_vma=False,
    )
```
